32 devices in a mesh: ep: 8 (over z, x), tp: 4 (over y, core).
Axes of the slice: x: 2, y: 2, z: 4, core: 2. Of those that a mesh axis runs over, the one named last changes fastest.
Arguments:
- hidden_in: bfloat16 [128, 4096], P('ep'), may hold values from -6 to 6
- w_query: bfloat16 [4096, 2048], P('ep', 'tp'), may hold values from -0.09375 to 0.09375
- w_key: bfloat16 [4096, 2048], P('ep', 'tp'), may hold values from -0.09375 to 0.09375
- w_value: bfloat16 [4096, 2048], P('ep', 'tp'), may hold values from -0.09375 to 0.09375
- w_outgate: bfloat16 [4096, 2048], P('ep', 'tp'), may hold values from -0.09375 to 0.09375
- w_igate: bfloat16 [4096, 16], P('ep', 'tp'), may hold values from -0.09375 to 0.09375
- w_fgate: bfloat16 [4096, 16], P('ep', 'tp'), may hold values from -0.09375 to 0.09375
- input_bias: float32 [16], P('tp'), may hold values from -3 to 303
- forget_bias: float32 [16], P('tp'), may hold values from -1 to 5
- mem_state: float32 [128, 16, 16384], P('ep', 'tp'), may hold values from -4 to 4
- max_state: float32 [128, 16], P('ep', 'tp'), may hold values from -4 to 304
- head_gain: float32 [2048], P('tp'), may hold values from 0.1 to 1.9
- w_output: bfloat16 [2048, 4096], P('tp'), may hold values from -0.26367188 to 0.26367188
- first_gain: float32 [4096], replicated, may hold values from 0.35 to 3.25
- w_group_router: bfloat16 [4096, 2], replicated, may hold values from -0.09375 to 0.09375
- w_expert_router: bfloat16 [4096, 8], replicated, may hold values from -0.09375 to 0.09375
- expert_route: int32 [128, 2], P('ep'), may hold values from 0 to 7, as said below
- w_expgate: bfloat16 [8, 4096, 1024], P('ep', None, 'tp'), may hold values from -0.09375 to 0.09375
- w_expup: bfloat16 [8, 4096, 1024], P('ep', None, 'tp'), may hold values from -0.09375 to 0.09375
- w_expdown: bfloat16 [8, 1024, 4096], P('ep', 'tp'), may hold values from -0.75 to 0.75
- second_gain: float32 [4096], P('tp'), may hold values from 0.1 to 1.9
Outputs:
- hidden_out: bfloat16 [128, 4096], P('ep', 'tp')
- mem_next: float32 [128, 16, 16384], P('ep', 'tp')
- max_next: float32 [128, 16], P('ep', 'tp')
The draws below stay inside these ranges and needn't reach their ends.
Inputs may be any that keep to these rules, and one draw needn't show every extreme that they name: `expert_route`: each row names two different experts of one group (an expert's group is its number divided by 4). In each aligned block of 16 rows (the rows of one index of ep) every group is named by exactly 8 rows, no expert by more than 8 rows, and some expert by exactly 8 rows.
All inputs are finite; a program needn't handle non-finite values.
Results may differ from the reference program's by a relative error of at most 0.02.
Values may be sent and summed in bfloat16 or wider, within the bound.
No kernel may reach another device: no remote copies, remote signals or barrier semaphores. Data moves between devices by JAX's collectives and lax.ppermute only.
A program may use at most 64 MiB of HBM per device.

```python
import jax
import jax.numpy as jnp
from jax import lax

D = 4096
HEADS = 16
DH = 128
HD = 2048
DE = 1024
GROUP_SIZE = 4
TOP_K = 2
EXPERTS = 8
GROUPS = 2
SEQ_DEV = 16
SEQUENCES = 128
CAP = 8
N_EP = 8
N_TP = 4


def draw_input_bias(key, part):
    base = jax.random.uniform(jax.random.fold_in(key, 1), (HEADS,), jnp.float32, -3.0, 3.0)
    return base


def draw_max_state(key, part):
    base = jax.random.uniform(jax.random.fold_in(key, 2), (SEQUENCES, HEADS), jnp.float32, -4.0, 4.0)
    return base


def draw_first_gain(key, part):
    positions = jnp.arange(D, dtype=jnp.float32) / D
    rough = jax.random.uniform(jax.random.fold_in(key, 3), (D,), jnp.float32, 0.7, 1.3)
    ramp = 0.5 * jnp.power(5.0, positions)
    return ramp * rough


def route_block(block_key):
    coin_key, forced_key, perm_key, swap_key, order_key = jax.random.split(block_key, 5)
    skewed = jax.random.randint(coin_key, (GROUPS,), 0, 2)
    forced = jax.random.randint(forced_key, (), 0, GROUPS)
    skewed = jnp.where(jnp.arange(GROUPS) == forced, 1, skewed)
    ranks_to_expert = jax.vmap(lambda one_key: jax.random.permutation(one_key, GROUP_SIZE))(jax.random.split(perm_key, GROUPS))
    skew_counts = jnp.array([CAP, 0, CAP // 2, CAP // 2], jnp.int32)
    even_counts = jnp.array([CAP // 2, CAP // 2, CAP // 2, CAP // 2], jnp.int32)
    counts = jnp.where(skewed[:, None] == 1, skew_counts[None, :], even_counts[None, :])
    running = jnp.cumsum(counts, 1)
    slots = jnp.arange(2 * CAP, dtype=jnp.int32)
    rank_of_slot = jnp.sum((slots[None, :, None] >= running[:, None, :]).astype(jnp.int32), -1)
    expert_of_slot = jnp.take_along_axis(ranks_to_expert, rank_of_slot, 1) + GROUP_SIZE * jnp.arange(GROUPS, dtype=jnp.int32)[:, None]
    pairs = jnp.stack([expert_of_slot[:, :CAP], expert_of_slot[:, CAP:]], -1).reshape(GROUPS * CAP, 2)
    swapped = jax.random.randint(swap_key, (GROUPS * CAP,), 0, 2)
    pairs = jnp.where(swapped[:, None] == 1, pairs[:, ::-1], pairs)
    order = jax.random.permutation(order_key, GROUPS * CAP)
    return pairs[order]


def draw_expert_route(key, part):
    block_keys = jax.random.split(jax.random.fold_in(key, 5), SEQUENCES // SEQ_DEV)
    routes = jax.vmap(route_block)(block_keys)
    return routes.reshape(SEQUENCES, TOP_K).astype(jnp.int32)


def shard_levels(rng, dims, cuts, least, largest):
    def one(position, parts):
        heights = jax.random.uniform(jax.random.fold_in(jax.random.fold_in(rng, 6), position), (parts,), jnp.float32, least / len(cuts), largest / len(cuts))
        return jnp.repeat(jnp.exp(heights), dims[position] // parts).reshape((-1,) + (1,) * (len(dims) - position - 1))

    level = one(*cuts[0])
    for cut in cuts[1:]:
        level = level * one(*cut)
    return level


def bell_draw(key, shape, deviation, reach, cuts=(), held_as=jnp.bfloat16):
    drawn = jax.random.normal(key, shape, jnp.float32) * deviation
    if len(cuts) > 0:
        drawn = shard_levels(key, shape, cuts, -0.22, 0.18) * drawn
    return jnp.clip(drawn, min=-reach, max=reach).astype(held_as)


def setup_inputs(seed: int = 0) -> dict:
    streams_of = jax.random.split(jax.random.key(seed), 22)
    return {
        "hidden_in": bell_draw(streams_of[0], (SEQUENCES, D), 1.0, 6.0, ((0, 8),)),
        "w_query": bell_draw(streams_of[1], (D, HD), D ** -0.5, 0.09375, ((0, 8), (1, 4))),
        "w_key": bell_draw(streams_of[2], (D, HD), D ** -0.5, 0.09375, ((0, 8), (1, 4))),
        "w_value": bell_draw(streams_of[3], (D, HD), D ** -0.5, 0.09375, ((0, 8), (1, 4))),
        "w_outgate": bell_draw(streams_of[4], (D, HD), D ** -0.5, 0.09375, ((0, 8), (1, 4))),
        "w_igate": bell_draw(streams_of[5], (D, HEADS), D ** -0.5, 0.09375, ((0, 8), (1, 4))),
        "w_fgate": bell_draw(streams_of[6], (D, HEADS), D ** -0.5, 0.09375, ((0, 8), (1, 4))),
        "input_bias": draw_input_bias(jax.random.fold_in(streams_of[21], 71), 0),
        "forget_bias": jnp.clip(-1.0 + 6.0 * jax.random.uniform(streams_of[8], (HEADS,), jnp.float32) ** shard_levels(streams_of[8], (HEADS,), ((0, 4),), -0.2, 0.2), -1.0, 5.0),
        "mem_state": bell_draw(streams_of[9], (SEQUENCES, HEADS, DH * DH), 0.5, 4.0, ((0, 8), (1, 4)), jnp.float32),
        "max_state": draw_max_state(jax.random.fold_in(streams_of[21], 71), 0),
        "head_gain": jnp.clip(1.0 + 0.18 * jax.random.normal(streams_of[11], (HD,), jnp.float32), 0.1, 1.9),
        "w_output": bell_draw(streams_of[12], (HD, D), (2.0 / HD ** 0.5), 0.26367188, ((0, 4),)),
        "first_gain": draw_first_gain(jax.random.fold_in(streams_of[21], 71), 0),
        "w_group_router": bell_draw(streams_of[14], (D, GROUPS), D ** -0.5, 0.09375),
        "w_expert_router": bell_draw(streams_of[15], (D, EXPERTS), D ** -0.5, 0.09375),
        "expert_route": draw_expert_route(jax.random.fold_in(streams_of[21], 71), 0),
        "w_expgate": bell_draw(streams_of[17], (EXPERTS, D, DE), D ** -0.5, 0.09375, ((0, 8), (2, 4))),
        "w_expup": bell_draw(streams_of[18], (EXPERTS, D, DE), D ** -0.5, 0.09375, ((0, 8), (2, 4))),
        "w_expdown": bell_draw(streams_of[19], (EXPERTS, DE, D), (4.0 / DE ** 0.5), 0.75, ((0, 8), (1, 4))),
        "second_gain": jnp.clip(1.0 + 0.18 * jax.random.normal(streams_of[20], (D,), jnp.float32), 0.1, 1.9),
    }


res_alpha = 8.0 ** 0.25

def layer_norm(values, gain):
    row_mean = lax.optimization_barrier(jnp.mean(values, -1, keepdims=True))
    row_var = lax.optimization_barrier(jnp.mean(values * values, -1, keepdims=True)) - row_mean * row_mean
    return (values - row_mean) * lax.rsqrt(row_var + 1e-05) * gain

def mlstm_step(queries, keys_scaled, values, log_input, log_forget, memory, stabilizer):
    new_max = jnp.maximum(log_forget + stabilizer, log_input)
    keep_old = jnp.exp(log_forget + stabilizer - new_max)
    write_new = jnp.exp(log_input - new_max)
    scores = lax.optimization_barrier(jnp.sum(queries * keys_scaled, -1)) * write_new
    read_old = jnp.einsum('bhd,bhde->bhe', queries, memory, precision=lax.Precision.HIGHEST)
    readout = scores[..., None] * values + keep_old[..., None] * read_old
    memory_next = keep_old[..., None, None] * memory + write_new[..., None, None] * keys_scaled[..., :, None] * values[..., None, :]
    return (readout, memory_next, new_max)

def head_mix(readout, head_gain, out_pre):
    scaled = readout * lax.rsqrt(lax.optimization_barrier(jnp.mean(readout * readout, -1, keepdims=True)) + 1e-06)
    flat_heads = scaled.reshape(scaled.shape[0], -1)
    return (flat_heads * head_gain * jax.nn.sigmoid(out_pre)).astype(jnp.bfloat16)

def route_weights(mid_float, w_group_router, w_expert_router, expert_route):
    group_logits = jnp.dot(mid_float, w_group_router.astype(jnp.float32), precision=lax.Precision.HIGHEST)
    expert_logits = jnp.dot(mid_float, w_expert_router.astype(jnp.float32), precision=lax.Precision.HIGHEST)
    first_expert = expert_route[:, 0]
    second_expert = expert_route[:, 1]
    expert_ids = lax.broadcasted_iota(jnp.int32, expert_logits.shape, 1)
    group_ids = lax.broadcasted_iota(jnp.int32, group_logits.shape, 1)
    first_logit = lax.optimization_barrier(jnp.sum(jnp.where(expert_ids == first_expert[:, None], expert_logits, 0.0), -1))
    second_logit = lax.optimization_barrier(jnp.sum(jnp.where(expert_ids == second_expert[:, None], expert_logits, 0.0), -1))
    group_pick = lax.optimization_barrier(jnp.sum(jnp.where(group_ids == (first_expert // GROUP_SIZE)[:, None], group_logits, 0.0), -1))
    group_gate = jax.nn.sigmoid(group_pick)
    return (group_gate * jax.nn.sigmoid(first_logit - second_logit), group_gate * jax.nn.sigmoid(second_logit - first_logit))

def slot_ranks(flat_routes, expert_total):
    onehot = (flat_routes[:, None] == lax.broadcasted_iota(jnp.int32, (flat_routes.shape[0], expert_total), 1)).astype(jnp.int32)
    running = jnp.cumsum(onehot, 0)
    return lax.optimization_barrier(jnp.sum((running - 1) * onehot, -1)).astype(jnp.int32)

def add_block(total, pieces):
    block_rows, block_weight = pieces
    partial_sum = jnp.dot(block_rows, block_weight, preferred_element_type=jnp.float32)
    partial_sum = lax.optimization_barrier(partial_sum.astype(jnp.bfloat16)).astype(jnp.float32)
    return (total + partial_sum, None)

def blocked_product(left, right):
    row_count = left.shape[0]
    inner = left.shape[1] // N_TP
    left_blocks = left.reshape(row_count, N_TP, inner).transpose(1, 0, 2)
    right_blocks = right.reshape(N_TP, inner, right.shape[1])
    total, unused = lax.scan(add_block, jnp.zeros((row_count, right.shape[1]), jnp.float32), (left_blocks, right_blocks))
    return total

def run_expert(pieces):
    rows_in, gate_weight, up_weight, down_weight = pieces
    gate_pre = jnp.dot(rows_in, gate_weight, preferred_element_type=jnp.float32)
    up_pre = jnp.dot(rows_in, up_weight, preferred_element_type=jnp.float32)
    hidden_units = (jax.nn.silu(gate_pre) * up_pre).astype(jnp.bfloat16)
    return blocked_product(hidden_units, down_weight).astype(jnp.bfloat16)

def reference(hidden_in, w_query, w_key, w_value, w_outgate, w_igate, w_fgate, input_bias, forget_bias, mem_state, max_state, head_gain, w_output, first_gain, w_group_router, w_expert_router, expert_route, w_expgate, w_expup, w_expdown, second_gain):
    shape4 = (SEQUENCES, HEADS, DH)
    queries = jnp.dot(hidden_in, w_query, preferred_element_type=jnp.float32).reshape(shape4)
    keys_scaled = jnp.dot(hidden_in, w_key, preferred_element_type=jnp.float32).reshape(shape4) * DH ** (-0.5)
    values = jnp.dot(hidden_in, w_value, preferred_element_type=jnp.float32).reshape(shape4)
    out_pre = jnp.dot(hidden_in, w_outgate, preferred_element_type=jnp.float32)
    log_input = jnp.dot(hidden_in, w_igate, preferred_element_type=jnp.float32) + input_bias
    log_forget = jax.nn.log_sigmoid(jnp.dot(hidden_in, w_fgate, preferred_element_type=jnp.float32) + forget_bias)
    memory = mem_state.reshape(SEQUENCES, HEADS, DH, DH)
    readout, mem_square, max_next = mlstm_step(queries, keys_scaled, values, log_input, log_forget, memory, max_state)
    mem_next = mem_square.reshape(SEQUENCES, HEADS, DH * DH)
    mixed_heads = head_mix(readout, head_gain, out_pre)
    mix = blocked_product(mixed_heads, w_output)
    mid_float = layer_norm(res_alpha * hidden_in.astype(jnp.float32) + mix, first_gain)
    mid = mid_float.astype(jnp.bfloat16)
    first_weight, second_weight = route_weights(mid_float, w_group_router, w_expert_router, expert_route)
    flat_routes = expert_route.reshape(-1).astype(jnp.int32)
    block_routes = flat_routes.reshape(N_EP, TOP_K * SEQ_DEV)
    ranks = jax.vmap(slot_ranks, in_axes=(0, None))(block_routes, EXPERTS).reshape(-1)
    source_block = (jnp.arange(SEQUENCES * TOP_K, dtype=jnp.int32) // (TOP_K * SEQ_DEV)).astype(jnp.int32)
    slot_index = ((flat_routes * N_EP + source_block) * CAP + ranks).astype(jnp.int32)
    repeated = jnp.repeat(mid, TOP_K, 0)
    buffer = jnp.zeros((EXPERTS * N_EP * CAP, D), jnp.bfloat16).at[slot_index].set(repeated)
    buffer = buffer.reshape(EXPERTS, N_EP * CAP, D)
    expert_out = lax.map(run_expert, (buffer, w_expgate, w_expup, w_expdown)).reshape(EXPERTS * N_EP * CAP, D)
    picked = expert_out[slot_index].astype(jnp.float32).reshape(SEQUENCES, TOP_K, D)
    moe = first_weight[:, None] * picked[:, 0] + second_weight[:, None] * picked[:, 1]
    joined = res_alpha * mid.astype(jnp.float32) + moe
    hidden_out = layer_norm(joined, second_gain).astype(jnp.bfloat16)
    return (hidden_out, mem_next, max_next)
```

```python
import jax
import jax.numpy as jnp
from jax import lax
from jax.experimental import pallas as pl
from jax.experimental.pallas import tpu as pltpu
from jax.sharding import PartitionSpec as P

D = 4096
DH = 128
GROUP_SIZE = 4


res_alpha = 8.0**0.25


def layer_norm(values, gain):
    row_mean = jnp.mean(values, -1, keepdims=True)
    row_var = jnp.mean(values * values, -1, keepdims=True) - row_mean * row_mean
    return (values - row_mean) * lax.rsqrt(row_var + 1e-05) * gain


def cell_kernel(
    input_bias_ref,
    forget_bias_ref,
    parts_ref,
    max_ref,
    gain_ref,
    memory_ref,
    mixed_ref,
    memory_out_ref,
    max_out_ref,
    query_s,
    key_s,
    value_s,
    gate_s,
    keep_s,
    write_s,
    mixed_s,
):
    step = pl.program_id(0)
    heads_here = memory_ref.shape[1]
    head_width = heads_here * DH
    rows = query_s.shape[0]

    @pl.when(step == 0)
    def prepare():
        total = parts_ref[0].astype(jnp.float32)
        for part in range(1, parts_ref.shape[0]):
            total = total + parts_ref[part].astype(jnp.float32)
        gates = total[:, 4 * head_width :]
        gated = gain_ref[...] * jax.nn.sigmoid(total[:, 3 * head_width : 4 * head_width])
        wide = (rows, DH)
        for h in range(heads_here):
            at = h * DH
            query_s[:, h : h + 1, :] = total[:, at : at + DH][:, None, :]
            key_s[:, h : h + 1, :] = (
                total[:, head_width + at : head_width + at + DH] * DH ** (-0.5)
            )[:, None, :]
            value_s[:, h : h + 1, :] = total[:, 2 * head_width + at : 2 * head_width + at + DH][
                :, None, :
            ]
            gate_s[:, h : h + 1, :] = gated[:, at : at + DH][:, None, :]
            f = heads_here + h
            low = 2 * heads_here
            input_sum = gates[:, h : h + 1] + gates[:, low + h : low + h + 1]
            forget_sum = gates[:, f : f + 1] + gates[:, low + f : low + f + 1]
            log_input = jnp.broadcast_to(input_sum, wide) + input_bias_ref[h]
            forget_pre = jnp.broadcast_to(forget_sum, wide) + forget_bias_ref[h]
            log_forget = jnp.minimum(forget_pre, 0.0) - jnp.log1p(jnp.exp(-jnp.abs(forget_pre)))
            carried = log_forget + jnp.broadcast_to(max_ref[:, h : h + 1], wide)
            new_max = jnp.maximum(carried, log_input)
            keep_s[:, h : h + 1, :] = jnp.exp(carried - new_max)[:, None, :]
            write_s[:, h : h + 1, :] = jnp.exp(log_input - new_max)[:, None, :]
            max_out_ref[:, h : h + 1] = new_max[:, 0:1]

    block = memory_ref.shape[0]
    for inner in range(block):
        row = step * block + inner
        query = query_s[row]
        key = key_s[row]
        value = value_s[row]
        keep = keep_s[row]
        write = write_s[row]
        write_key = write * key
        sums = [jnp.zeros_like(query) for _ in range(4)]
        for d in range(DH):
            old = memory_ref[inner, :, d * DH : (d + 1) * DH]
            sums[d % 4] = sums[d % 4] + query[:, d : d + 1] * old
            memory_out_ref[inner, :, d * DH : (d + 1) * DH] = (
                keep * old + write_key[:, d : d + 1] * value
            )
        read_old = (sums[0] + sums[1]) + (sums[2] + sums[3])
        scores = jnp.sum(query * key, -1, keepdims=True) * write
        readout = scores * value + keep * read_old
        scaled = readout * lax.rsqrt(jnp.mean(readout * readout, -1, keepdims=True) + 1e-06)
        mixed_s[row] = scaled * gate_s[row]

    @pl.when(step == pl.num_programs(0) - 1)
    def finish():
        for h in range(heads_here):
            mixed_ref[:, h * DH : (h + 1) * DH] = mixed_s[:, h, :].astype(jnp.bfloat16)


def cell(parts, input_bias, forget_bias, mem_state, max_state, head_gain):
    rows, heads_here, square = mem_state.shape
    head_width = heads_here * DH
    block = 2 if rows % 2 == 0 else 1
    fixed = lambda shape: pl.BlockSpec(shape, lambda i: (0,) * len(shape))
    moving = pl.BlockSpec((block, heads_here, square), lambda i: (i, 0, 0))
    scratch = pltpu.VMEM((rows, heads_here, DH), jnp.float32)
    return pl.pallas_call(
        cell_kernel,
        grid=(rows // block,),
        in_specs=[
            pl.BlockSpec(memory_space=pltpu.SMEM),
            pl.BlockSpec(memory_space=pltpu.SMEM),
            fixed(parts.shape),
            fixed(max_state.shape),
            fixed((1, head_width)),
            moving,
        ],
        out_specs=[fixed((rows, head_width)), moving, fixed(max_state.shape)],
        out_shape=[
            jax.ShapeDtypeStruct((rows, head_width), jnp.bfloat16),
            jax.ShapeDtypeStruct(mem_state.shape, jnp.float32),
            jax.ShapeDtypeStruct(max_state.shape, jnp.float32),
        ],
        scratch_shapes=[scratch] * 7,
        compiler_params=pltpu.CompilerParams(
            dimension_semantics=("arbitrary",), vmem_limit_bytes=16 * 1024 * 1024
        ),
        name="cell",
    )(input_bias, forget_bias, parts, max_state, head_gain.reshape(1, -1), mem_state)


def exchange(blocks, axes):
    return lax.all_to_all(blocks, axes, split_axis=0, concat_axis=0, tiled=True)


def route_weights(mid_float, w_group_router, w_expert_router, expert_route):
    group_logits = jnp.dot(
        mid_float, w_group_router.astype(jnp.float32), precision=lax.Precision.HIGHEST
    )
    expert_logits = jnp.dot(
        mid_float, w_expert_router.astype(jnp.float32), precision=lax.Precision.HIGHEST
    )
    first_expert = expert_route[:, 0]
    second_expert = expert_route[:, 1]
    expert_ids = lax.broadcasted_iota(jnp.int32, expert_logits.shape, 1)
    group_ids = lax.broadcasted_iota(jnp.int32, group_logits.shape, 1)
    first_logit = jnp.sum(jnp.where(expert_ids == first_expert[:, None], expert_logits, 0.0), -1)
    second_logit = jnp.sum(jnp.where(expert_ids == second_expert[:, None], expert_logits, 0.0), -1)
    group_pick = jnp.sum(
        jnp.where(group_ids == (first_expert // GROUP_SIZE)[:, None], group_logits, 0.0), -1
    )
    group_gate = jax.nn.sigmoid(group_pick)
    return (
        group_gate * jax.nn.sigmoid(first_logit - second_logit),
        group_gate * jax.nn.sigmoid(second_logit - first_logit),
    )


def slot_ranks(flat_routes, expert_total):
    onehot = (
        flat_routes[:, None]
        == lax.broadcasted_iota(jnp.int32, (flat_routes.shape[0], expert_total), 1)
    ).astype(jnp.int32)
    running = jnp.cumsum(onehot, 0)
    return jnp.sum((running - 1) * onehot, -1)


def body(
    hidden_in,
    w_query,
    w_key,
    w_value,
    w_outgate,
    w_igate,
    w_fgate,
    input_bias,
    forget_bias,
    mem_state,
    max_state,
    head_gain,
    w_output,
    first_gain,
    w_group_router,
    w_expert_router,
    expert_route,
    w_expgate,
    w_expup,
    w_expdown,
    second_gain,
):
    own_rows, width = hidden_in.shape
    heads_here = mem_state.shape[1]
    head_width = heads_here * DH
    top_count = expert_route.shape[1]
    ep_size = lax.axis_size("ep")
    tp_size = lax.axis_size("tp")
    spread_rows = exchange(
        hidden_in.reshape(own_rows, ep_size, width // ep_size).transpose(1, 0, 2), "ep"
    ).reshape(own_rows * ep_size, width // ep_size)
    stacked_w = jnp.concatenate([w_query, w_key, w_value, w_outgate], 1)
    gate_w = jnp.concatenate([w_igate, w_fgate], 1)
    proj_terms = jnp.dot(spread_rows, stacked_w, preferred_element_type=jnp.float32)
    gate_terms = jnp.dot(spread_rows, gate_w, preferred_element_type=jnp.float32)
    gate_high = lax.reduce_precision(gate_terms, 8, 7)
    gate_low = gate_terms - gate_high
    gate_pad = jnp.zeros((own_rows * ep_size, -4 * heads_here % DH), jnp.bfloat16)
    terms = jnp.concatenate(
        [
            proj_terms.astype(jnp.bfloat16),
            gate_high.astype(jnp.bfloat16),
            gate_low.astype(jnp.bfloat16),
            gate_pad,
        ],
        1,
    )
    parts = exchange(terms.reshape(ep_size, own_rows, terms.shape[1]), "ep")
    mixed_heads, memory_next, new_max = cell(
        parts, input_bias, forget_bias, mem_state, max_state, head_gain
    )
    partial_mix = jnp.dot(mixed_heads, w_output, preferred_element_type=jnp.float32).astype(
        jnp.bfloat16
    )
    mix = jnp.sum(lax.all_gather(partial_mix, "tp").astype(jnp.float32), 0)
    mid_float = layer_norm(res_alpha * hidden_in.astype(jnp.float32) + mix, first_gain)
    mid = mid_float.astype(jnp.bfloat16)
    first_weight, second_weight = route_weights(
        mid_float, w_group_router, w_expert_router, expert_route
    )
    expert_total = w_expgate.shape[0] * ep_size
    capacity = 2 * own_rows * top_count // expert_total
    flat_routes = expert_route.reshape(-1)
    local_slot = flat_routes * capacity + slot_ranks(flat_routes, expert_total)
    share_width = width // tp_size
    mid_share = lax.dynamic_slice_in_dim(mid, lax.axis_index("tp") * share_width, share_width, 1)
    slots = lax.broadcasted_iota(jnp.int32, (expert_total * capacity, own_rows), 0)
    slot_of = local_slot.reshape(own_rows, top_count)
    picks = slots == slot_of[:, 0][None, :]
    for choice in range(1, top_count):
        picks = picks | (slots == slot_of[:, choice][None, :])
    buffer = jnp.dot(picks.astype(jnp.bfloat16), mid, preferred_element_type=jnp.float32).astype(
        jnp.bfloat16
    )
    experts_here = w_expgate.shape[0]
    arrived = (
        exchange(buffer.reshape(ep_size, experts_here * capacity, width), "ep")
        .reshape(ep_size, experts_here, capacity, width)
        .transpose(1, 0, 2, 3)
        .reshape(experts_here, ep_size * capacity, width)
    )
    gate_pre = jnp.einsum("erd,edf->erf", arrived, w_expgate, preferred_element_type=jnp.float32)
    up_pre = jnp.einsum("erd,edf->erf", arrived, w_expup, preferred_element_type=jnp.float32)
    hidden_units = (jax.nn.silu(gate_pre) * up_pre).astype(jnp.bfloat16)
    down_terms = jnp.einsum(
        "erf,efd->erd", hidden_units, w_expdown, preferred_element_type=jnp.float32
    ).astype(jnp.bfloat16)
    outgoing = (
        down_terms.reshape(experts_here, ep_size, capacity, tp_size, share_width)
        .transpose(1, 3, 0, 2, 4)
        .reshape(ep_size * tp_size, experts_here * capacity, share_width)
    )
    returned = exchange(outgoing, ("ep", "tp")).reshape(
        ep_size, tp_size, experts_here * capacity, share_width
    )
    expert_out = (
        jnp.sum(returned.astype(jnp.float32), 1)
        .astype(jnp.bfloat16)
        .reshape(expert_total * capacity, share_width)
    )
    chosen = local_slot[None, :] == lax.broadcasted_iota(
        jnp.int32, (expert_total * capacity, own_rows * top_count), 0
    )
    picked = lax.dot_general(
        chosen.astype(jnp.bfloat16),
        expert_out,
        (((0,), (0,)), ((), ())),
        preferred_element_type=jnp.float32,
    )
    picked = picked.reshape(own_rows, top_count, share_width)
    moe = first_weight[:, None] * picked[:, 0] + second_weight[:, None] * picked[:, 1]
    joined = res_alpha * mid_share.astype(jnp.float32) + moe
    sums = jnp.stack([jnp.sum(joined, -1), jnp.sum(joined * joined, -1)])
    row_sum, square_sum = jnp.sum(lax.all_gather(sums, "tp"), 0)
    row_mean = row_sum / D
    row_var = square_sum / D - row_mean * row_mean
    hidden_out = (
        (joined - row_mean[:, None]) * lax.rsqrt(row_var[:, None] + 1e-05) * second_gain
    ).astype(jnp.bfloat16)
    return (hidden_out, memory_next, new_max)


def solution(mesh):
    return jax.shard_map(
        body,
        mesh=mesh,
        in_specs=(
            P("ep", None),
            P("ep", "tp"),
            P("ep", "tp"),
            P("ep", "tp"),
            P("ep", "tp"),
            P("ep", "tp"),
            P("ep", "tp"),
            P("tp"),
            P("tp"),
            P("ep", "tp", None),
            P("ep", "tp"),
            P("tp"),
            P("tp", None),
            P(),
            P(),
            P(),
            P("ep", None),
            P("ep", None, "tp"),
            P("ep", None, "tp"),
            P("ep", "tp", None),
            P("tp"),
        ),
        out_specs=(P("ep", "tp"), P("ep", "tp", None), P("ep", "tp")),
        check_vma=False,
    )
```
